128 devices in a mesh: tp: 16 (over z, x), dp: 8 (over y, core).
Axes of the slice: x: 4, y: 4, z: 4, core: 2. Of those that a mesh axis runs over, the one named last changes fastest.
Arguments:
- tokens: bfloat16 [224, 4096], P('tp', 'dp'), may hold values from -6 to 6
- w_query: bfloat16 [2, 4096, 4096], P(None, 'dp', 'tp'), may hold values from -0.09375 to 0.09375
- w_key: bfloat16 [2, 4096, 4096], P(None, 'dp', 'tp'), may hold values from -0.09375 to 0.09375
- w_value: bfloat16 [2, 4096, 4096], P(None, 'dp', 'tp'), may hold values from -0.09375 to 0.09375
- w_outgate: bfloat16 [2, 4096, 4096], P(None, 'dp', 'tp'), may hold values from -0.09375 to 0.09375
- w_ingate: bfloat16 [2, 4096, 32], P(None, 'dp'), may hold values from -0.09375 to 0.09375
- w_forget: bfloat16 [2, 4096, 32], P(None, 'dp'), may hold values from -0.09375 to 0.09375
- forget_bias: float32 [2, 32], P(None, 'tp'), may hold values from -2 to 3
- head_gain: float32 [2, 32, 128], P(None, 'tp'), may hold values from 0.1 to 1.9
- w_proj: bfloat16 [2, 4096, 4096], P(None, 'tp', 'dp'), may hold values from -0.09375 to 0.09375
- mem_matrix: float32 [2, 224, 32, 128, 128], P(None, 'dp', 'tp'), may hold values from -0.8 to 0.8
- mem_norm: float32 [2, 224, 32, 128], P(None, 'dp', 'tp'), may hold values from -1.2 to 1.2
- mem_max: float32 [2, 224, 32], P(None, 'dp', 'tp'), may hold values from -4 to 4
Outputs:
- result: bfloat16 [224, 4096], P('tp', 'dp')
- new_matrix: float32 [2, 224, 32, 128, 128], P(None, 'dp', 'tp')
- new_norm: float32 [2, 224, 32, 128], P(None, 'dp', 'tp')
- new_max: float32 [2, 224, 32], P(None, 'dp', 'tp')
The draws below stay inside these ranges and needn't reach their ends.
All inputs are finite; a program needn't handle non-finite values.
Results may differ from the reference program's by a relative error of at most 0.017.
Values may be sent and summed in bfloat16 or wider, within the bound.
A program may use at most 128 MiB of HBM per device.

```python
import jax
import jax.numpy as jnp
from jax import lax

D = 4096
HEADS = 32
HEAD = 128
BLOCKS = 2
BATCH = 224


def level_of(key, shape, pieces, low, largest):
    def one(position, blocks):
        draws = jax.random.uniform(jax.random.fold_in(jax.random.fold_in(key, 6), position), (blocks,), jnp.float32, low / len(pieces), largest / len(pieces))
        return jnp.repeat(jnp.exp(draws), shape[position] // blocks).reshape((-1,) + (1,) * (len(shape) - position - 1))

    loudness = one(*pieces[0])
    for cut in pieces[1:]:
        loudness = loudness * one(*cut)
    return loudness


def gaussian(stream_key, shape, deviation, limit, cuts=(), held_as=jnp.bfloat16):
    level = level_of(stream_key, shape, cuts, -0.22, 0.18) if cuts else 1.0
    array = jax.random.normal(stream_key, shape, jnp.float32) * deviation * level
    return jnp.minimum(jnp.maximum(array, -limit), limit).astype(held_as)


def setup_inputs(seed: int = 0) -> dict:
    keys = jax.random.split(jax.random.key(seed), 14)
    return {
        "tokens": gaussian(keys[0], (BATCH, D), 1.0, 6.0, ((0, 16), (1, 8))),
        "w_query": gaussian(keys[1], (BLOCKS, D, D), D ** -0.5, 0.09375, ((1, 8), (2, 16))),
        "w_key": gaussian(keys[2], (BLOCKS, D, D), D ** -0.5, 0.09375, ((1, 8), (2, 16))),
        "w_value": gaussian(keys[3], (BLOCKS, D, D), D ** -0.5, 0.09375, ((1, 8), (2, 16))),
        "w_outgate": gaussian(keys[4], (BLOCKS, D, D), D ** -0.5, 0.09375, ((1, 8), (2, 16))),
        "w_ingate": gaussian(keys[5], (BLOCKS, D, HEADS), D ** -0.5, 0.09375, ((1, 8),)),
        "w_forget": gaussian(keys[6], (BLOCKS, D, HEADS), D ** -0.5, 0.09375, ((1, 8),)),
        "forget_bias": jnp.clip(-2.0 + 5.0 * jax.random.uniform(keys[7], (BLOCKS, HEADS), jnp.float32) ** level_of(keys[7], (BLOCKS, HEADS), ((1, 16),), -0.2, 0.2), -2.0, 3.0),
        "head_gain": jnp.clip(1.0 + 0.18 * jax.random.normal(keys[8], (BLOCKS, HEADS, HEAD), jnp.float32), 0.1, 1.9),
        "w_proj": gaussian(keys[9], (BLOCKS, D, D), D ** -0.5, 0.09375, ((1, 16), (2, 8))),
        "mem_matrix": gaussian(keys[10], (BLOCKS, BATCH, HEADS, HEAD, HEAD), 0.1, 0.8, ((1, 8), (2, 16)), jnp.float32),
        "mem_norm": gaussian(keys[11], (BLOCKS, BATCH, HEADS, HEAD), 0.15, 1.2, ((1, 8), (2, 16)), jnp.float32),
        "mem_max": gaussian(keys[12], (BLOCKS, BATCH, HEADS), 1.0, 4.0, ((1, 8), (2, 16)), jnp.float32),
    }


norm_eps = 1e-06
head_eps = 1e-05

def full_sum(x_rows, weight):
    return jnp.dot(x_rows, weight, preferred_element_type=jnp.float32)

def cell_update(queries, key_vecs, values, log_in, log_forget, matrix, normvec, maxval):
    max_next = jnp.maximum(log_forget + maxval, log_in)
    decays = jnp.exp(log_forget + maxval - max_next)
    weight_in = jnp.exp(log_in - max_next)
    matrix_new = decays[..., None, None] * matrix + weight_in[..., None, None] * key_vecs[..., :, None] * values[..., None, :]
    norm_new = decays[..., None] * normvec + weight_in[..., None] * key_vecs
    numerator = jnp.einsum('bhd,bhde->bhe', queries, matrix_new, precision=lax.Precision.HIGHEST)
    denominator = jnp.maximum(jnp.abs(lax.optimization_barrier(jnp.sum(queries * norm_new, axis=-1))), 1.0)
    return (numerator / denominator[..., None], matrix_new, norm_new, max_next)

def head_norm(readout, gain, outgate):
    average = lax.optimization_barrier(jnp.mean(readout, axis=-1, keepdims=True))
    variance = lax.optimization_barrier(jnp.mean(jnp.square(readout - average), axis=-1, keepdims=True))
    normed = (readout - average) * lax.rsqrt(variance + head_eps) * gain
    return normed * jax.nn.sigmoid(outgate)

def mix_block(x_rows, weights, states):
    w_query, w_key, w_value, w_outgate, w_ingate, w_forget, bias, gain, w_proj = weights
    matrix, normvec, maxval = states
    row_count, features = x_rows.shape
    squares = lax.optimization_barrier(jnp.sum(jnp.square(x_rows.astype(jnp.float32)), axis=1))
    inv_scale = lax.rsqrt(squares / features + norm_eps)[:, None]
    head_shape = (row_count, HEADS, HEAD)
    queries = (full_sum(x_rows, w_query) * inv_scale).reshape(head_shape)
    key_vecs = (full_sum(x_rows, w_key) * inv_scale * HEAD ** (-0.5)).reshape(head_shape)
    values = (full_sum(x_rows, w_value) * inv_scale).reshape(head_shape)
    outgate = (full_sum(x_rows, w_outgate) * inv_scale).reshape(head_shape)
    log_in = full_sum(x_rows, w_ingate) * inv_scale
    log_forget = jax.nn.log_sigmoid(full_sum(x_rows, w_forget) * inv_scale + bias[None, :])
    readout, matrix_new, norm_new, max_next = cell_update(queries, key_vecs, values, log_in, log_forget, matrix, normvec, maxval)
    hidden = head_norm(readout, gain[None], outgate).reshape(row_count, -1).astype(jnp.bfloat16)
    mixed_out = jnp.dot(hidden, w_proj, preferred_element_type=jnp.float32).astype(jnp.bfloat16)
    return (mixed_out, matrix_new, norm_new, max_next)

def reference(tokens, w_query, w_key, w_value, w_outgate, w_ingate, w_forget, forget_bias, head_gain, w_proj, mem_matrix, mem_norm, mem_max):
    current = tokens
    matrix_list, norm_list, max_list = ([], [], [])
    for block_id in range(BLOCKS):
        weights = (w_query[block_id], w_key[block_id], w_value[block_id], w_outgate[block_id], w_ingate[block_id], w_forget[block_id], forget_bias[block_id], head_gain[block_id], w_proj[block_id])
        current, matrix_out, norm_out, max_out = mix_block(current, weights, (mem_matrix[block_id], mem_norm[block_id], mem_max[block_id]))
        matrix_list.append(matrix_out)
        norm_list.append(norm_out)
        max_list.append(max_out)
    return (current, jnp.stack(matrix_list), jnp.stack(norm_list), jnp.stack(max_list))
```

```python
import functools

import jax
import jax.numpy as jnp
from jax import lax
from jax.experimental import pallas as pl
from jax.experimental.pallas import tpu as pltpu
from jax.sharding import PartitionSpec as P

HEAD = 128
CELLS = 2
norm_eps = 1e-06
head_eps = 1e-05
MESH = pl.DeviceIdType.MESH
F32 = jnp.float32
BF16 = jnp.bfloat16
ORDER = (2, 1, 3, 0)
OTHERS = (2, 1, 3)


def remote(src, dst, send, recv, tp, dp):
    return pltpu.make_async_remote_copy(
        src_ref=src,
        dst_ref=dst,
        send_sem=send,
        recv_sem=recv,
        device_id={"tp": tp, "dp": dp},
        device_id_type=MESH,
    )


NH = 2
RB = 16 // NH
V = 14 // NH
R2 = 2 * RB
GROUPS = (
    (("q",), ("k",), ("v", "o")),
    (("q",), ("k",), ("v", "o")),
)
EXACT = ({"q", "k", "v", "o"}, {"q"})
WIDE = (F32, BF16)
WROWS = (V, RB)
WNAMES = ("q", "k", "v", "o", "i", "f", "p")


def group_type(cell, group):
    return F32 if group[0] in EXACT[cell] else BF16


def group_shape(cell, group):
    rows = V if group_type(cell, group) == F32 and group[0] != "q" else RB
    return (NH, 4, len(group), 2, rows, 256)


def kernel(*refs):
    (tok, wq, wk, wv, wo, wi, wf, bias, gain, wp, mem, nrm, mxs) = refs[:13]
    res_out, mb, nb, mxb = refs[13:17]
    rest = list(refs[17:])
    take = lambda n: [rest.pop(0) for _ in range(n)]
    (tokb, biasb, gainb, xo, xb, wb, gb, wpb, gsel, hb, mh, ml,
     npad, mxt, mxpad, dec_s, kt_s, v_s, q_s, rd_s, pad_s) = take(21)
    ob, orb = take(2), take(2)
    ps, rs = [], []
    for cell in range(CELLS):
        ps.append(take(len(GROUPS[cell])))
        rs.append(take(len(GROUPS[cell])))
    (ag_s, ag_r, rs_s, rs_r, h_s, h_r, o_s, o_r, wl, ws, wr, m_i, s_i, t_i) = take(14)

    t = lax.axis_index("tp")
    d = lax.axis_index("dp")
    z, x = t // 4, t % 4
    y, c = d // 2, d % 2
    other = 2 * y + (1 - c)
    cs = x // 2
    mine = 2 * z + x % 2

    def own_weight(cell, i):
        if i < 4:
            return (wq, wk, wv, wo)[i].at[cell], wb.at[cell, c, i]
        if i < 6:
            return (wi, wf)[i - 4].at[cell], gb.at[cell, c, i - 4]
        return wp.at[cell], wpb.at[cell, c]

    def local_weight(cell, i):
        src, dst = own_weight(cell, i)
        return pltpu.make_async_copy(src, dst, wl.at[cell, i])

    def pair_weight(cell, i):
        src, dst = own_weight(cell, i)
        return remote(src, dst, ws.at[cell, i], wr.at[cell, i], t, other)

    def have_weight(cell, i):
        local_weight(cell, i).wait()
        pair_weight(cell, i).wait_recv()

    def states_in(cell):
        return (
            pltpu.make_async_copy(nrm.at[cell], nb.at[cell], s_i.at[cell, 0]),
            pltpu.make_async_copy(mxs.at[cell], mxb.at[cell], s_i.at[cell, 1]),
            pltpu.make_async_copy(mem.at[cell], mb.at[cell], m_i.at[cell]),
        )

    small = (
        pltpu.make_async_copy(tok, tokb, t_i.at[0]),
        pltpu.make_async_copy(bias, biasb, t_i.at[1]),
        pltpu.make_async_copy(gain, gainb, t_i.at[2]),
    )
    for cp in small:
        cp.start()

    barrier = pltpu.get_barrier_semaphore()

    def greet(tp, dp):
        pl.semaphore_signal(barrier, inc=1, device_id={"tp": tp, "dp": dp}, device_id_type=MESH)

    for dz in ORDER:
        for dx in ORDER:
            t2 = ((z + dz) % 4) * 4 + (x + dx) % 4
            if dz == 0 and dx == 0:
                greet(t, other)
            else:
                greet(t2, 2 * y)
                greet(t2, 2 * y + 1)
    for dy in (2, 1, 3):
        greet(t, 2 * ((y + dy) % 4) + c)

    for i in (4, 5, 0, 1, 2, 3, 6):
        local_weight(0, i).start()
    for cp in states_in(0):
        cp.start()

    xo[...] = jnp.zeros_like(xo)
    npad[...] = jnp.zeros_like(npad)
    mxt[...] = jnp.zeros_like(mxt)
    rd_s[...] = jnp.zeros_like(rd_s)
    pad_s[...] = jnp.zeros_like(pad_s)
    for cp in small:
        cp.wait()
    for hf in range(NH):
        xo[0, hf, 0:V, :] = tokb[V * hf:V * hf + V, :]

    pl.semaphore_wait(barrier, 34)

    def gather(cell, hf):
        out = []
        k = 0
        for dz in ORDER:
            for dx in ORDER:
                t2 = ((z + dz) % 4) * 4 + (x + dx) % 4
                cp = remote(
                    xo.at[cell, hf], xb.at[cell, hf, c, mine], ag_s.at[cell, hf, k], ag_r.at[cell, hf, c, mine],
                    t2, 2 * y + cs,
                )
                out.append((cp, cs != c if dz == 0 and dx == 0 else None))
                k += 1
        return out

    def gather_in(cell, hf):
        out = []
        for c2 in range(2):
            for j in range(8):
                t2 = 4 * (j // 2) + 2 * c + j % 2
                cp = remote(
                    xo.at[cell, hf], xb.at[cell, hf, c2, j], ag_s.at[cell, hf, 0], ag_r.at[cell, hf, c2, j],
                    t2, 2 * y + c2,
                )
                out.append((cp, jnp.logical_or(t2 != t, c2 != c)))
        return out

    def spread(cell, hf, k):
        out = []
        for b in range(2):
            x2 = 2 * c + b
            for c2 in range(2):
                cp = remote(
                    ob[cell].at[hf, c2, 2 * k + b], orb[cell].at[hf, t],
                    o_s.at[cell, hf, 4 * k + 2 * b + c2], o_r.at[cell, hf, t], 4 * k + x2, 2 * y + c2,
                )
                out.append((cp, jnp.logical_or(jnp.logical_or(k != z, x2 != x), c2 != c)))
        return out

    def spread_in(cell, hf):
        out = []
        for t2 in range(16):
            cp = remote(
                ob[cell].at[hf, 0, 0], orb[cell].at[hf, t2], o_s.at[cell, hf, 0], o_r.at[cell, hf, t2], t2, 2 * y + cs
            )
            out.append((cp, jnp.logical_or(t != t2, cs != c)))
        return out

    def across(cell, hf, n):
        src, dst = ps[cell][n], rs[cell][n]
        out = []
        for dy in (2, 1, 3):
            y2 = (y + dy) % 4
            out.append(remote(
                src.at[hf, y2], dst.at[hf, y], rs_s.at[cell, hf, n, dy], rs_r.at[cell, hf, n, y], t, 2 * y2 + c
            ))
        return out

    def across_in(cell, hf, n):
        src, dst = ps[cell][n], rs[cell][n]
        out = []
        for dy in (1, 3, 2):
            y2 = (y + dy) % 4
            out.append(remote(
                src.at[hf, y], dst.at[hf, y2], rs_s.at[cell, hf, n, dy], rs_r.at[cell, hf, n, y2], t, 2 * y2 + c
            ))
        return out

    def hid(cell, hf):
        return [
            remote(hb.at[cell, hf, y], hb.at[cell, hf, y], h_s.at[cell, hf, dy], h_r.at[cell, hf, y],
                   t, 2 * ((y + dy) % 4) + c)
            for dy in (2, 1, 3)
        ]

    def hid_in(cell, hf):
        out = []
        for dy in (1, 3, 2):
            y2 = (y + dy) % 4
            out.append(remote(
                hb.at[cell, hf, y], hb.at[cell, hf, y2], h_s.at[cell, hf, dy], h_r.at[cell, hf, y2], t, 2 * y2 + c
            ))
        return out

    def each(pairs, what):
        for cp, cond in pairs:
            if cond is None:
                getattr(cp, what)()
            else:
                @pl.when(cond)
                def _():
                    getattr(cp, what)()

    for hf in range(NH):
        each(gather(0, hf), "start")
    for i in (4, 5, 0, 1, 2, 3, 6):
        pair_weight(0, i).start()
    for cp in states_in(1):
        cp.start()
    for i in range(7):
        local_weight(1, i).start()
    for i in range(7):
        pair_weight(1, i).start()

    row = lax.broadcasted_iota(jnp.int32, (R2, HEAD), 0)
    pad_row = lax.broadcasted_iota(jnp.int32, (R2, 256), 0) == V
    gate_row = lax.broadcasted_iota(jnp.int32, (HEAD, 512), 0)
    ones_at = jnp.where(gate_row // R2 == 4, 1.0, 0.0).astype(BF16)
    own_lane = lax.broadcasted_iota(jnp.int32, (R2, HEAD), 1) % R2 == row

    def nt(a, b):
        return lax.dot_general(a, b, (((1,), (1,)), ((), ())), preferred_element_type=F32)

    def prepare(cell):
        have_weight(cell, 4)
        have_weight(cell, 5)
        for g in range(2):
            want = lax.broadcasted_iota(jnp.int32, (HEAD, 32), 0) // R2 - 2 * g
            head = lax.broadcasted_iota(jnp.int32, (HEAD, 32), 1)
            pick = jnp.logical_and(jnp.logical_and(want >= 0, want < 2), head == 2 * t + want)
            pick = jnp.where(pick, 1.0, 0.0).astype(BF16)
            for c2 in range(2):
                part = jnp.dot(pick, gb[cell, c2, g], preferred_element_type=F32).astype(BF16)
                if g == 0:
                    gsel[cell, c2] = part
                else:
                    gsel[cell, c2] = gsel[cell, c2] + part
        cps = states_in(cell)
        for cp in cps:
            cp.wait()
        for hf in range(NH):
            for s in range(2):
                at = 14 * s + V * hf
                mxt[cell, hf, 0:2, RB * s:RB * s + V] = mxb[cell, :, at:at + V]
                for h in range(2):
                    npad[cell, hf, h, RB * s:RB * s + V, :] = nb[cell, pl.ds(2 * at + h, V, stride=2), :]
            mxpad[cell, hf] = mxt[cell, hf].T

        def split(b, carry):
            for h in range(2):
                m = mb[cell, b, h]
                high = m.astype(BF16)
                mh[cell, b, h] = high
                if cell == 0:
                    ml[b, h] = (m - high.astype(F32)).astype(BF16)
            return carry

        lax.fori_loop(0, 28, split, 0, unroll=2)

    def project(cell, parts):
        for hf in parts:
            @pl.when(cs == c)
            def _():
                xb[cell, hf, c, mine] = xo[cell, hf]

        for hf in parts:
            each(gather_in(cell, hf), "wait_recv")
        x0, x1 = (
            jnp.concatenate([xb[cell, hf, c2].reshape(8 * RB, 512) for hf in parts], axis=0) for c2 in range(2)
        )
        gates = nt(x0, gsel[cell, 0]) + nt(x1, gsel[cell, 1]) + nt(x0 * x0, ones_at) + nt(x1 * x1, ones_at)
        gates = gates.reshape(len(parts), 4, R2, HEAD)
        gates = jnp.sum(jnp.where(own_lane[None, None], gates, 0.0), axis=2, keepdims=True)
        for n, group in enumerate(GROUPS[cell]):
            dst = ps[cell][n]
            for m, name in enumerate(group):
                i = WNAMES.index(name)
                if parts[0] == 0:
                    have_weight(cell, i)
                acc = jnp.dot(x0, wb[cell, 0, i], preferred_element_type=F32)
                acc += jnp.dot(x1, wb[cell, 1, i], preferred_element_type=F32)
                acc = acc.astype(dst.dtype).reshape(len(parts), 4, 2, RB, 256)
                for k, hf in enumerate(parts):
                    dst[hf, :, m] = acc[k, :, :, 0:dst.shape[4]]
                    if name == "q":
                        dst[hf, :, m, 0, V:V + 1, 0:HEAD] = gates[k]
            for hf in parts:
                for cp in across(cell, hf, n):
                    cp.start()

    def total(cell, hf, name):
        for n, group in enumerate(GROUPS[cell]):
            if name not in group:
                continue
            if name == group[0]:
                for cp in across_in(cell, hf, n):
                    cp.wait_recv()
            m = group.index(name)
            ref = rs[cell][n]
            mine_ref = ps[cell][n]
            out = mine_ref[hf, y, m].astype(F32)
            for dy in (1, 2, 3):
                out = out + ref[hf, (y + dy) % 4, m].astype(F32)
            if out.shape[1] == RB:
                return out.reshape(R2, 256)
            for s in range(2):
                pad_s[cell, hf, WNAMES.index(name) - 1, RB * s:RB * s + V] = out[s]
            return pad_s[cell, hf, WNAMES.index(name) - 1]

    def heads(cell, hf):
        queries = total(cell, hf, "q")
        flat = jnp.where(own_lane, jnp.broadcast_to(queries[V:V + 1, 0:HEAD], (R2, HEAD)), 0.0)
        which = lax.broadcasted_iota(jnp.int32, (R2, HEAD), 1) // R2
        gate = [jnp.sum(jnp.where(which == k, flat, 0.0), axis=1, keepdims=True) for k in range(5)]
        queries = jnp.where(pad_row, 0.0, queries)
        inv = lax.rsqrt(gate[4] / 4096 + norm_eps)
        decs, wins = [], []
        for h in range(2):
            log_in = gate[h] * inv
            f = gate[2 + h] * inv + biasb[cell, h]
            log_forget = jnp.minimum(f, 0.0) - jnp.log1p(jnp.exp(-jnp.abs(f)))
            old = log_forget + mxpad[cell, hf, 0:R2, h:h + 1]
            new = jnp.maximum(old, log_in)
            mxpad[cell, hf, 0:R2, h:h + 1] = new
            decs.append(jnp.exp(old - new))
            wins.append(jnp.exp(log_in - new))
            dec_s[cell, hf, h] = jnp.broadcast_to(decs[h], (R2, HEAD))
        queries = queries * inv
        keys = total(cell, hf, "k") * inv * HEAD ** (-0.5)
        alphas, dens = [], []
        for h in range(2):
            qh = queries[:, HEAD * h:HEAD * (h + 1)]
            q_s[h] = qh
            wkey = keys[:, HEAD * h:HEAD * (h + 1)] * wins[h]
            kt_s[cell, hf, h] = wkey.T.astype(BF16)
            new = decs[h] * npad[cell, hf, h] + wkey
            npad[cell, hf, h] = new
            alphas.append(jnp.sum(qh * wkey, axis=-1, keepdims=True))
            dens.append(jnp.maximum(jnp.abs(jnp.sum(qh * new, axis=-1, keepdims=True)), 1.0))

        for s in range(2):
            for i in range(V):
                r = RB * s + i
                b = 14 * s + V * hf + i
                for h in range(2):
                    q_row = jnp.broadcast_to(q_s[h, r:r + 1, :], (8, HEAD))
                    q_high = q_row.astype(BF16).astype(F32)
                    both = jnp.concatenate([q_high, q_row - q_high], axis=0).astype(BF16)
                    read = jnp.dot(both, mh[cell, b, h], preferred_element_type=F32)
                    if cell == 0:
                        read = read[0:8] + read[8:16] + jnp.dot(both, ml[b, h], preferred_element_type=F32)[0:8]
                    rd_s[h, r:r + 1, :] = read[0:1]

        values = total(cell, hf, "v") * inv
        outgate = total(cell, hf, "o") * inv
        for h in range(2):
            value = values[:, HEAD * h:HEAD * (h + 1)]
            v_s[cell, hf, h] = value
            read = (decs[h] * rd_s[h] + alphas[h] * value) / dens[h]
            mean = jnp.mean(read, axis=-1, keepdims=True)
            var = jnp.mean(jnp.square(read - mean), axis=-1, keepdims=True)
            normed = (read - mean) * lax.rsqrt(var + head_eps) * gainb[cell, h:h + 1, :]
            hidden = normed * jax.nn.sigmoid(outgate[:, HEAD * h:HEAD * (h + 1)])
            hb[cell, hf, y, :, HEAD * h:HEAD * (h + 1)] = hidden.astype(BF16)
        for cp in hid(cell, hf):
            cp.start()
        if hf == 0:
            have_weight(cell, 6)
        out_pieces(cell, hf, (0,))
        each(spread(cell, hf, y), "start")

    def out_pieces(cell, hf, dys):
        ks = [(y + dy) % 4 for dy in dys]
        hid_rows = jnp.concatenate([hb[cell, hf, k] for k in ks], axis=0)
        for c2 in range(2):
            acc = jnp.dot(hid_rows, wpb[cell, c2], preferred_element_type=F32)
            acc = acc.astype(WIDE[cell]).reshape(len(dys), 2, RB, 512)[:, :, 0:WROWS[cell]]
            for at, k in enumerate(ks):
                ob[cell][hf, c2, pl.ds(2 * k, 2)] = acc[at]

    def outputs(cell, hf):
        for cp in hid_in(cell, hf):
            cp.wait_recv()
        out_pieces(cell, hf, OTHERS)
        for dz in ORDER:
            z2 = (z + dz) % 4
            for cp, cond in spread(cell, hf, z2):
                @pl.when(jnp.logical_and(z2 != y, cond))
                def _():
                    cp.start()

        @pl.when(cs == c)
        def _():
            orb[cell][hf, t] = ob[cell][hf, c, mine]

    def update(cell):
        for hf in range(NH):
            mxt[cell, hf] = mxpad[cell, hf].T
            for s in range(2):
                at = 14 * s + V * hf
                mxb[cell, :, at:at + V] = mxt[cell, hf, 0:2, RB * s:RB * s + V]
                for h in range(2):
                    nb[cell, pl.ds(2 * at + h, V, stride=2), :] = npad[cell, hf, h, RB * s:RB * s + V, :]

            def one(i, carry):
                for s in range(2):
                    r = RB * s + i
                    b = 14 * s + V * hf + i
                    for h in range(2):
                        v_row = jnp.where(row == r, v_s[cell, hf, h], 0.0).astype(BF16)
                        outer = jnp.dot(kt_s[cell, hf, h], v_row, preferred_element_type=F32)
                        mb[cell, b, h] = dec_s[cell, hf, h, pl.ds(r, 1), :] * mb[cell, b, h] + outer
                return carry

            lax.fori_loop(0, V, one, 0)

    def collect(cell, hf):
        each(spread_in(cell, hf), "wait_recv")
        tot = orb[cell][hf, 0].astype(F32)
        for t2 in range(1, 16):
            tot += orb[cell][hf, t2].astype(F32)
        xo[cell + 1, hf, 0:WROWS[cell]] = tot.astype(BF16)
        if cell + 1 < CELLS:
            each(gather(cell + 1, hf), "start")

    def settle(cell):
        for hf in range(NH):
            each(gather(cell, hf), "wait_send")
            if cell:
                for k in range(4):
                    each(spread(cell - 1, hf, k), "wait_send")
            for n in range(len(GROUPS[cell])):
                for cp in across(cell, hf, n):
                    cp.wait_send()
            for cp in hid(cell, hf):
                cp.wait_send()
        for i in range(7):
            pair_weight(cell, i).wait_send()

    prepare(0)
    for cell in range(CELLS):
        for parts in [(hf,) for hf in range(NH)]:
            project(cell, parts)
        for hf in range(NH):
            heads(cell, hf)
        for hf in range(NH):
            outputs(cell, hf)
        update(cell)
        if cell + 1 < CELLS:
            prepare(cell + 1)
        settle(cell)
        for hf in range(NH):
            collect(cell, hf)
    for hf in range(NH):
        res_out[V * hf:V * hf + V, :] = xo[CELLS, hf, 0:V, :]

    for hf in range(NH):
        for k in range(4):
            each(spread(CELLS - 1, hf, k), "wait_send")


def flush(res, mb, nb, mxb, res_out, mem_out, nrm_out, mxs_out, sems):
    cps = [
        pltpu.make_async_copy(
            mb.at[i // 4, pl.ds(7 * (i % 4), 7)], mem_out.at[i // 4, pl.ds(7 * (i % 4), 7)], sems.at[i]
        )
        for i in range(8)
    ]
    cps.append(pltpu.make_async_copy(res, res_out, sems.at[8]))
    cps.append(pltpu.make_async_copy(nb, nrm_out, sems.at[9]))
    cps.append(pltpu.make_async_copy(mxb, mxs_out, sems.at[10]))
    for cp in cps:
        cp.start()
    for cp in cps:
        cp.wait()


def on_device(tokens, wq, wk, wv, wo, wi, wf, bias, gain, wp, mem, nrm, mxs):
    hbm = pl.BlockSpec(memory_space=pltpu.HBM)
    vmem = pl.BlockSpec(memory_space=pltpu.VMEM)
    dma = pltpu.SemaphoreType.DMA
    nrm2 = nrm.reshape(CELLS, 56, HEAD)
    mxs2 = mxs.transpose(0, 2, 1)
    wi2 = wi.transpose(0, 2, 1)
    wf2 = wf.transpose(0, 2, 1)
    shapes = (
        jax.ShapeDtypeStruct((14, 512), BF16),
        jax.ShapeDtypeStruct(mem.shape, F32),
        jax.ShapeDtypeStruct(nrm2.shape, F32),
        jax.ShapeDtypeStruct(mxs2.shape, F32),
    )
    held = pl.pallas_call(
        kernel,
        out_shape=tuple(pltpu.VMEM(a.shape, a.dtype) for a in shapes),
        in_specs=[hbm] * 13,
        out_specs=(vmem,) * 4,
        scratch_shapes=[
            pltpu.VMEM((14, 512), BF16),
            pltpu.SMEM((CELLS, 2), F32),
            pltpu.VMEM((CELLS, 2, HEAD), F32),
            pltpu.VMEM((CELLS + 1, NH, RB, 512), BF16),
            pltpu.VMEM((CELLS, NH, 2, 8, RB, 512), BF16),
            pltpu.VMEM((CELLS, 2, 4, 512, 256), BF16),
            pltpu.VMEM((CELLS, 2, 2, 32, 512), BF16),
            pltpu.VMEM((CELLS, 2, 256, 512), BF16),
            pltpu.VMEM((CELLS, 2, HEAD, 512), BF16),
            pltpu.VMEM((CELLS, NH, 4, R2, 256), BF16),
            pltpu.VMEM((CELLS, 28, 2, HEAD, HEAD), BF16),
            pltpu.VMEM((28, 2, HEAD, HEAD), BF16),
            pltpu.VMEM((CELLS, NH, 2, R2, HEAD), F32),
            pltpu.VMEM((CELLS, NH, 8, HEAD), F32),
            pltpu.VMEM((CELLS, NH, HEAD, 8), F32),
            pltpu.VMEM((CELLS, NH, 2, R2, HEAD), F32),
            pltpu.VMEM((CELLS, NH, 2, HEAD, R2), BF16),
            pltpu.VMEM((CELLS, NH, 2, R2, HEAD), F32),
            pltpu.VMEM((2, R2, HEAD), F32),
            pltpu.VMEM((2, R2, HEAD), F32),
            pltpu.VMEM((1, NH, 3, R2, 256), F32),
            *(pltpu.VMEM((NH, 2, 8, WROWS[cell], 512), WIDE[cell]) for cell in range(CELLS)),
            *(pltpu.VMEM((NH, 16, WROWS[cell], 512), WIDE[cell]) for cell in range(CELLS)),
            *(
                pltpu.VMEM(group_shape(cell, group), group_type(cell, group))
                for cell in range(CELLS) for _ in range(2) for group in GROUPS[cell]
            ),
            dma((CELLS, NH, 16)), dma((CELLS, NH, 2, 8)),
            dma((CELLS, NH, 4, 4)), dma((CELLS, NH, 4, 4)),
            dma((CELLS, NH, 4)), dma((CELLS, NH, 4)),
            dma((CELLS, NH, 16)), dma((CELLS, NH, 16)),
            dma((CELLS, 7)), dma((CELLS, 7)), dma((CELLS, 7)),
            dma((CELLS,)), dma((CELLS, 2)), dma((3,)),
        ],
        compiler_params=pltpu.CompilerParams(
            collective_id=0, has_side_effects=True, vmem_limit_bytes=48 * 1024 * 1024
        ),
    )(*(pltpu.with_memory_space_constraint(a, pltpu.HBM) for a in (tokens, wq, wk, wv, wo, wi2, wf2, bias, gain, wp, mem, nrm2, mxs2)))
    res, mem_new, nrm_new, mxs_new = pl.pallas_call(
        flush,
        out_shape=shapes,
        in_specs=[vmem] * 4,
        out_specs=(hbm,) * 4,
        scratch_shapes=[dma((11,))],
        compiler_params=pltpu.CompilerParams(vmem_limit_bytes=1024 * 1024),
    )(*held)
    return res, mem_new, nrm_new.reshape(nrm.shape), mxs_new.transpose(0, 2, 1)


def solution(mesh):
    in_specs = (
        P("tp", "dp"),
        P(None, "dp", "tp"),
        P(None, "dp", "tp"),
        P(None, "dp", "tp"),
        P(None, "dp", "tp"),
        P(None, "dp", None),
        P(None, "dp", None),
        P(None, "tp"),
        P(None, "tp", None),
        P(None, "tp", "dp"),
        P(None, "dp", "tp", None, None),
        P(None, "dp", "tp", None),
        P(None, "dp", "tp"),
    )
    out_specs = (
        P("tp", "dp"),
        P(None, "dp", "tp", None, None),
        P(None, "dp", "tp", None),
        P(None, "dp", "tp"),
    )
    return jax.shard_map(on_device, mesh=mesh, in_specs=in_specs, out_specs=out_specs, check_vma=False)
```

```python
import functools

import jax
import jax.numpy as jnp
from jax import lax
from jax.experimental import pallas as pl
from jax.experimental.pallas import tpu as pltpu
from jax.sharding import PartitionSpec as P

HEAD = 128
CELLS = 2
norm_eps = 1e-06
head_eps = 1e-05
MESH = pl.DeviceIdType.MESH
F32 = jnp.float32
BF16 = jnp.bfloat16
ORDER = (2, 1, 3, 0)
OTHERS = (2, 1, 3)


def remote(src, dst, send, recv, tp, dp):
    return pltpu.make_async_remote_copy(
        src_ref=src,
        dst_ref=dst,
        send_sem=send,
        recv_sem=recv,
        device_id={"tp": tp, "dp": dp},
        device_id_type=MESH,
    )


NH = 2
RB = 16 // NH
V = 14 // NH
R2 = 2 * RB
GROUPS = (
    (("q",), ("k",), ("v", "o")),
    (("q",), ("k",), ("v", "o")),
)
EXACT = ({"q", "k", "v", "o"}, {"q"})
WIDE = (F32, BF16)
WROWS = (V, RB)
WNAMES = ("q", "k", "v", "o", "i", "f", "p")


def group_type(cell, group):
    return F32 if group[0] in EXACT[cell] else BF16


def group_shape(cell, group):
    rows = V if group_type(cell, group) == F32 and group[0] != "q" else RB
    return (NH, 4, len(group), 2, rows, 256)


def kernel(*refs):
    (tok, wq, wk, wv, wo, wi, wf, bias, gain, wp, mem, nrm, mxs) = refs[:13]
    res_out, mb, nb, mxb = refs[13:17]
    rest = list(refs[17:])
    take = lambda n: [rest.pop(0) for _ in range(n)]
    (tokb, biasb, gainb, xo, xb, wb, gb, wpb, gsel, hb, mh, ml,
     npad, mxt, mxpad, dec_s, kt_s, v_s, q_s, rd_s, pad_s) = take(21)
    ob, orb = take(2), take(2)
    ps, rs = [], []
    for cell in range(CELLS):
        ps.append(take(len(GROUPS[cell])))
        rs.append(take(len(GROUPS[cell])))
    (ag_s, ag_r, rs_s, rs_r, h_s, h_r, o_s, o_r, wl, ws, wr, m_i, s_i, t_i) = take(14)

    t = lax.axis_index("tp")
    d = lax.axis_index("dp")
    z, x = t // 4, t % 4
    y, c = d // 2, d % 2
    other = 2 * y + (1 - c)
    cs = x // 2
    mine = 2 * z + x % 2

    def own_weight(cell, i):
        if i < 4:
            return (wq, wk, wv, wo)[i].at[cell], wb.at[cell, c, i]
        if i < 6:
            return (wi, wf)[i - 4].at[cell], gb.at[cell, c, i - 4]
        return wp.at[cell], wpb.at[cell, c]

    def local_weight(cell, i):
        src, dst = own_weight(cell, i)
        return pltpu.make_async_copy(src, dst, wl.at[cell, i])

    def pair_weight(cell, i):
        src, dst = own_weight(cell, i)
        return remote(src, dst, ws.at[cell, i], wr.at[cell, i], t, other)

    def have_weight(cell, i):
        local_weight(cell, i).wait()
        pair_weight(cell, i).wait_recv()

    def states_in(cell):
        return (
            pltpu.make_async_copy(nrm.at[cell], nb.at[cell], s_i.at[cell, 0]),
            pltpu.make_async_copy(mxs.at[cell], mxb.at[cell], s_i.at[cell, 1]),
            pltpu.make_async_copy(mem.at[cell], mb.at[cell], m_i.at[cell]),
        )

    small = (
        pltpu.make_async_copy(tok, tokb, t_i.at[0]),
        pltpu.make_async_copy(bias, biasb, t_i.at[1]),
        pltpu.make_async_copy(gain, gainb, t_i.at[2]),
    )
    for cp in small:
        cp.start()

    barrier = pltpu.get_barrier_semaphore()

    def greet(tp, dp):
        pl.semaphore_signal(barrier, inc=1, device_id={"tp": tp, "dp": dp}, device_id_type=MESH)

    for dz in ORDER:
        for dx in ORDER:
            t2 = ((z + dz) % 4) * 4 + (x + dx) % 4
            if dz == 0 and dx == 0:
                greet(t, other)
            else:
                greet(t2, 2 * y)
                greet(t2, 2 * y + 1)
    for dy in (2, 1, 3):
        greet(t, 2 * ((y + dy) % 4) + c)

    for i in (4, 5, 0, 1, 2, 3, 6):
        local_weight(0, i).start()
    for cp in states_in(0):
        cp.start()

    xo[...] = jnp.zeros_like(xo)
    npad[...] = jnp.zeros_like(npad)
    mxt[...] = jnp.zeros_like(mxt)
    rd_s[...] = jnp.zeros_like(rd_s)
    pad_s[...] = jnp.zeros_like(pad_s)
    for cp in small:
        cp.wait()
    for hf in range(NH):
        xo[0, hf, 0:V, :] = tokb[V * hf:V * hf + V, :]

    pl.semaphore_wait(barrier, 34)

    def gather(cell, hf):
        out = []
        k = 0
        for dz in ORDER:
            for dx in ORDER:
                t2 = ((z + dz) % 4) * 4 + (x + dx) % 4
                cp = remote(
                    xo.at[cell, hf], xb.at[cell, hf, c, mine], ag_s.at[cell, hf, k], ag_r.at[cell, hf, c, mine],
                    t2, 2 * y + cs,
                )
                out.append((cp, cs != c if dz == 0 and dx == 0 else None))
                k += 1
        return out

    def gather_in(cell, hf):
        out = []
        for c2 in range(2):
            for j in range(8):
                t2 = 4 * (j // 2) + 2 * c + j % 2
                cp = remote(
                    xo.at[cell, hf], xb.at[cell, hf, c2, j], ag_s.at[cell, hf, 0], ag_r.at[cell, hf, c2, j],
                    t2, 2 * y + c2,
                )
                out.append((cp, jnp.logical_or(t2 != t, c2 != c)))
        return out

    def spread(cell, hf, k):
        out = []
        for b in range(2):
            x2 = 2 * c + b
            for c2 in range(2):
                cp = remote(
                    ob[cell].at[hf, c2, 2 * k + b], orb[cell].at[hf, t],
                    o_s.at[cell, hf, 4 * k + 2 * b + c2], o_r.at[cell, hf, t], 4 * k + x2, 2 * y + c2,
                )
                out.append((cp, jnp.logical_or(jnp.logical_or(k != z, x2 != x), c2 != c)))
        return out

    def spread_in(cell, hf):
        out = []
        for t2 in range(16):
            cp = remote(
                ob[cell].at[hf, 0, 0], orb[cell].at[hf, t2], o_s.at[cell, hf, 0], o_r.at[cell, hf, t2], t2, 2 * y + cs
            )
            out.append((cp, jnp.logical_or(t != t2, cs != c)))
        return out

    def across(cell, hf, n):
        src, dst = ps[cell][n], rs[cell][n]
        out = []
        for dy in (2, 1, 3):
            y2 = (y + dy) % 4
            out.append(remote(
                src.at[hf, y2], dst.at[hf, y], rs_s.at[cell, hf, n, dy], rs_r.at[cell, hf, n, y], t, 2 * y2 + c
            ))
        return out

    def across_in(cell, hf, n):
        src, dst = ps[cell][n], rs[cell][n]
        out = []
        for dy in (1, 3, 2):
            y2 = (y + dy) % 4
            out.append(remote(
                src.at[hf, y], dst.at[hf, y2], rs_s.at[cell, hf, n, dy], rs_r.at[cell, hf, n, y2], t, 2 * y2 + c
            ))
        return out

    def hid(cell, hf):
        return [
            remote(hb.at[cell, hf, y], hb.at[cell, hf, y], h_s.at[cell, hf, dy], h_r.at[cell, hf, y],
                   t, 2 * ((y + dy) % 4) + c)
            for dy in (2, 1, 3)
        ]

    def hid_in(cell, hf):
        out = []
        for dy in (1, 3, 2):
            y2 = (y + dy) % 4
            out.append(remote(
                hb.at[cell, hf, y], hb.at[cell, hf, y2], h_s.at[cell, hf, dy], h_r.at[cell, hf, y2], t, 2 * y2 + c
            ))
        return out

    def each(pairs, what):
        for cp, cond in pairs:
            if cond is None:
                getattr(cp, what)()
            else:
                @pl.when(cond)
                def _():
                    getattr(cp, what)()

    each(gather(0, 0), "start")
    for i in (4, 5, 0, 1, 2, 3, 6):
        pair_weight(0, i).start()
    for hf in range(1, NH):
        each(gather(0, hf), "start")
    for cp in states_in(1):
        cp.start()
    for i in range(7):
        local_weight(1, i).start()
    for i in range(7):
        pair_weight(1, i).start()

    row = lax.broadcasted_iota(jnp.int32, (R2, HEAD), 0)
    pad_row = lax.broadcasted_iota(jnp.int32, (R2, 256), 0) == V
    gate_row = lax.broadcasted_iota(jnp.int32, (HEAD, 512), 0)
    ones_at = jnp.where(gate_row // R2 == 4, 1.0, 0.0).astype(BF16)
    own_lane = lax.broadcasted_iota(jnp.int32, (R2, HEAD), 1) % R2 == row

    def nt(a, b):
        return lax.dot_general(a, b, (((1,), (1,)), ((), ())), preferred_element_type=F32)

    def prepare(cell):
        have_weight(cell, 4)
        have_weight(cell, 5)
        for g in range(2):
            want = lax.broadcasted_iota(jnp.int32, (HEAD, 32), 0) // R2 - 2 * g
            head = lax.broadcasted_iota(jnp.int32, (HEAD, 32), 1)
            pick = jnp.logical_and(jnp.logical_and(want >= 0, want < 2), head == 2 * t + want)
            pick = jnp.where(pick, 1.0, 0.0).astype(BF16)
            for c2 in range(2):
                part = jnp.dot(pick, gb[cell, c2, g], preferred_element_type=F32).astype(BF16)
                if g == 0:
                    gsel[cell, c2] = part
                else:
                    gsel[cell, c2] = gsel[cell, c2] + part
        cps = states_in(cell)
        for cp in cps:
            cp.wait()
        for hf in range(NH):
            for s in range(2):
                at = 14 * s + V * hf
                mxt[cell, hf, 0:2, RB * s:RB * s + V] = mxb[cell, :, at:at + V]
                for h in range(2):
                    npad[cell, hf, h, RB * s:RB * s + V, :] = nb[cell, pl.ds(2 * at + h, V, stride=2), :]
            mxpad[cell, hf] = mxt[cell, hf].T

        def split(b, carry):
            for h in range(2):
                m = mb[cell, b, h]
                high = m.astype(BF16)
                mh[cell, b, h] = high
                if cell == 0:
                    ml[b, h] = (m - high.astype(F32)).astype(BF16)
            return carry

        lax.fori_loop(0, 28, split, 0, unroll=2)

    def project(cell, parts):
        for hf in parts:
            @pl.when(cs == c)
            def _():
                xb[cell, hf, c, mine] = xo[cell, hf]

        for hf in parts:
            each(gather_in(cell, hf), "wait_recv")
        x0, x1 = (
            jnp.concatenate([xb[cell, hf, c2].reshape(8 * RB, 512) for hf in parts], axis=0) for c2 in range(2)
        )
        gates = nt(x0, gsel[cell, 0]) + nt(x1, gsel[cell, 1]) + nt(x0 * x0, ones_at) + nt(x1 * x1, ones_at)
        gates = gates.reshape(len(parts), 4, R2, HEAD)
        gates = jnp.sum(jnp.where(own_lane[None, None], gates, 0.0), axis=2, keepdims=True)
        for n, group in enumerate(GROUPS[cell]):
            dst = ps[cell][n]
            for m, name in enumerate(group):
                i = WNAMES.index(name)
                if parts[0] == 0:
                    have_weight(cell, i)
                acc = jnp.dot(x0, wb[cell, 0, i], preferred_element_type=F32)
                acc += jnp.dot(x1, wb[cell, 1, i], preferred_element_type=F32)
                acc = acc.astype(dst.dtype).reshape(len(parts), 4, 2, RB, 256)
                for k, hf in enumerate(parts):
                    dst[hf, :, m] = acc[k, :, :, 0:dst.shape[4]]
                    if name == "q":
                        dst[hf, :, m, 0, V:V + 1, 0:HEAD] = gates[k]
            for hf in parts:
                for cp in across(cell, hf, n):
                    cp.start()

    def total(cell, hf, name):
        for n, group in enumerate(GROUPS[cell]):
            if name not in group:
                continue
            if name == group[0]:
                for cp in across_in(cell, hf, n):
                    cp.wait_recv()
            m = group.index(name)
            ref = rs[cell][n]
            mine_ref = ps[cell][n]
            out = mine_ref[hf, y, m].astype(F32)
            for dy in (1, 2, 3):
                out = out + ref[hf, (y + dy) % 4, m].astype(F32)
            if out.shape[1] == RB:
                return out.reshape(R2, 256)
            for s in range(2):
                pad_s[cell, hf, WNAMES.index(name) - 1, RB * s:RB * s + V] = out[s]
            return pad_s[cell, hf, WNAMES.index(name) - 1]

    def heads(cell, hf):
        queries = total(cell, hf, "q")
        flat = jnp.where(own_lane, jnp.broadcast_to(queries[V:V + 1, 0:HEAD], (R2, HEAD)), 0.0)
        which = lax.broadcasted_iota(jnp.int32, (R2, HEAD), 1) // R2
        gate = [jnp.sum(jnp.where(which == k, flat, 0.0), axis=1, keepdims=True) for k in range(5)]
        queries = jnp.where(pad_row, 0.0, queries)
        inv = lax.rsqrt(gate[4] / 4096 + norm_eps)
        decs, wins = [], []
        for h in range(2):
            log_in = gate[h] * inv
            f = gate[2 + h] * inv + biasb[cell, h]
            log_forget = jnp.minimum(f, 0.0) - jnp.log1p(jnp.exp(-jnp.abs(f)))
            old = log_forget + mxpad[cell, hf, 0:R2, h:h + 1]
            new = jnp.maximum(old, log_in)
            mxpad[cell, hf, 0:R2, h:h + 1] = new
            decs.append(jnp.exp(old - new))
            wins.append(jnp.exp(log_in - new))
            dec_s[cell, hf, h] = jnp.broadcast_to(decs[h], (R2, HEAD))
        queries = queries * inv
        for h in range(2):
            q_s[h] = queries[:, HEAD * h:HEAD * (h + 1)]
        for s in range(2):
            for i in range(V):
                r = RB * s + i
                b = 14 * s + V * hf + i
                for h in range(2):
                    q_row = jnp.broadcast_to(q_s[h, r:r + 1, :], (8, HEAD))
                    q_high = q_row.astype(BF16).astype(F32)
                    both = jnp.concatenate([q_high, q_row - q_high], axis=0).astype(BF16)
                    read = jnp.dot(both, mh[cell, b, h], preferred_element_type=F32)
                    if cell == 0:
                        read = read[0:8] + read[8:16] + jnp.dot(both, ml[b, h], preferred_element_type=F32)[0:8]
                    rd_s[h, r:r + 1, :] = read[0:1]

        keys = total(cell, hf, "k") * inv * HEAD ** (-0.5)
        alphas, dens = [], []
        for h in range(2):
            qh = queries[:, HEAD * h:HEAD * (h + 1)]
            wkey = keys[:, HEAD * h:HEAD * (h + 1)] * wins[h]
            kt_s[cell, hf, h] = wkey.T.astype(BF16)
            new = decs[h] * npad[cell, hf, h] + wkey
            npad[cell, hf, h] = new
            alphas.append(jnp.sum(qh * wkey, axis=-1, keepdims=True))
            dens.append(jnp.maximum(jnp.abs(jnp.sum(qh * new, axis=-1, keepdims=True)), 1.0))

        values = total(cell, hf, "v") * inv
        outgate = total(cell, hf, "o") * inv
        for h in range(2):
            value = values[:, HEAD * h:HEAD * (h + 1)]
            v_s[cell, hf, h] = value
            read = (decs[h] * rd_s[h] + alphas[h] * value) / dens[h]
            mean = jnp.mean(read, axis=-1, keepdims=True)
            var = jnp.mean(jnp.square(read - mean), axis=-1, keepdims=True)
            normed = (read - mean) * lax.rsqrt(var + head_eps) * gainb[cell, h:h + 1, :]
            hidden = normed * jax.nn.sigmoid(outgate[:, HEAD * h:HEAD * (h + 1)])
            hb[cell, hf, y, :, HEAD * h:HEAD * (h + 1)] = hidden.astype(BF16)
        for cp in hid(cell, hf):
            cp.start()
        if hf == 0:
            have_weight(cell, 6)
        out_pieces(cell, hf, (0,))
        each(spread(cell, hf, y), "start")

    def out_pieces(cell, hf, dys):
        ks = [(y + dy) % 4 for dy in dys]
        hid_rows = jnp.concatenate([hb[cell, hf, k] for k in ks], axis=0)
        for c2 in range(2):
            acc = jnp.dot(hid_rows, wpb[cell, c2], preferred_element_type=F32)
            acc = acc.astype(WIDE[cell]).reshape(len(dys), 2, RB, 512)[:, :, 0:WROWS[cell]]
            for at, k in enumerate(ks):
                ob[cell][hf, c2, pl.ds(2 * k, 2)] = acc[at]

    def outputs(cell, hf):
        for cp in hid_in(cell, hf):
            cp.wait_recv()
        out_pieces(cell, hf, OTHERS)
        for dz in ORDER:
            z2 = (z + dz) % 4
            for cp, cond in spread(cell, hf, z2):
                @pl.when(jnp.logical_and(z2 != y, cond))
                def _():
                    cp.start()

        @pl.when(cs == c)
        def _():
            orb[cell][hf, t] = ob[cell][hf, c, mine]

    def update(cell):
        for hf in range(NH):
            mxt[cell, hf] = mxpad[cell, hf].T
            for s in range(2):
                at = 14 * s + V * hf
                mxb[cell, :, at:at + V] = mxt[cell, hf, 0:2, RB * s:RB * s + V]
                for h in range(2):
                    nb[cell, pl.ds(2 * at + h, V, stride=2), :] = npad[cell, hf, h, RB * s:RB * s + V, :]

            def one(i, carry):
                for s in range(2):
                    r = RB * s + i
                    b = 14 * s + V * hf + i
                    for h in range(2):
                        v_row = jnp.where(row == r, v_s[cell, hf, h], 0.0).astype(BF16)
                        outer = jnp.dot(kt_s[cell, hf, h], v_row, preferred_element_type=F32)
                        mb[cell, b, h] = dec_s[cell, hf, h, pl.ds(r, 1), :] * mb[cell, b, h] + outer
                return carry

            lax.fori_loop(0, V, one, 0)

    def collect(cell, hf):
        each(spread_in(cell, hf), "wait_recv")
        tot = orb[cell][hf, 0].astype(F32)
        for t2 in range(1, 16):
            tot += orb[cell][hf, t2].astype(F32)
        xo[cell + 1, hf, 0:WROWS[cell]] = tot.astype(BF16)
        if cell + 1 < CELLS:
            each(gather(cell + 1, hf), "start")

    def settle(cell):
        for hf in range(NH):
            each(gather(cell, hf), "wait_send")
            if cell:
                for k in range(4):
                    each(spread(cell - 1, hf, k), "wait_send")
            for n in range(len(GROUPS[cell])):
                for cp in across(cell, hf, n):
                    cp.wait_send()
            for cp in hid(cell, hf):
                cp.wait_send()
        for i in range(7):
            pair_weight(cell, i).wait_send()

    prepare(0)
    for cell in range(CELLS):
        for parts in [(hf,) for hf in range(NH)]:
            project(cell, parts)
        for hf in range(NH):
            heads(cell, hf)
        for hf in range(NH):
            outputs(cell, hf)
        update(cell)
        if cell + 1 < CELLS:
            prepare(cell + 1)
        settle(cell)
        for hf in range(NH):
            collect(cell, hf)
    for hf in range(NH):
        res_out[V * hf:V * hf + V, :] = xo[CELLS, hf, 0:V, :]

    for hf in range(NH):
        for k in range(4):
            each(spread(CELLS - 1, hf, k), "wait_send")


def flush(res, mb, nb, mxb, res_out, mem_out, nrm_out, mxs_out, sems):
    cps = [
        pltpu.make_async_copy(
            mb.at[i // 4, pl.ds(7 * (i % 4), 7)], mem_out.at[i // 4, pl.ds(7 * (i % 4), 7)], sems.at[i]
        )
        for i in range(8)
    ]
    cps.append(pltpu.make_async_copy(res, res_out, sems.at[8]))
    cps.append(pltpu.make_async_copy(nb, nrm_out, sems.at[9]))
    cps.append(pltpu.make_async_copy(mxb, mxs_out, sems.at[10]))
    for cp in cps:
        cp.start()
    for cp in cps:
        cp.wait()


def on_device(tokens, wq, wk, wv, wo, wi, wf, bias, gain, wp, mem, nrm, mxs):
    hbm = pl.BlockSpec(memory_space=pltpu.HBM)
    vmem = pl.BlockSpec(memory_space=pltpu.VMEM)
    dma = pltpu.SemaphoreType.DMA
    nrm2 = nrm.reshape(CELLS, 56, HEAD)
    mxs2 = mxs.transpose(0, 2, 1)
    wi2 = wi.transpose(0, 2, 1)
    wf2 = wf.transpose(0, 2, 1)
    shapes = (
        jax.ShapeDtypeStruct((14, 512), BF16),
        jax.ShapeDtypeStruct(mem.shape, F32),
        jax.ShapeDtypeStruct(nrm2.shape, F32),
        jax.ShapeDtypeStruct(mxs2.shape, F32),
    )
    held = pl.pallas_call(
        kernel,
        out_shape=tuple(pltpu.VMEM(a.shape, a.dtype) for a in shapes),
        in_specs=[hbm] * 13,
        out_specs=(vmem,) * 4,
        scratch_shapes=[
            pltpu.VMEM((14, 512), BF16),
            pltpu.SMEM((CELLS, 2), F32),
            pltpu.VMEM((CELLS, 2, HEAD), F32),
            pltpu.VMEM((CELLS + 1, NH, RB, 512), BF16),
            pltpu.VMEM((CELLS, NH, 2, 8, RB, 512), BF16),
            pltpu.VMEM((CELLS, 2, 4, 512, 256), BF16),
            pltpu.VMEM((CELLS, 2, 2, 32, 512), BF16),
            pltpu.VMEM((CELLS, 2, 256, 512), BF16),
            pltpu.VMEM((CELLS, 2, HEAD, 512), BF16),
            pltpu.VMEM((CELLS, NH, 4, R2, 256), BF16),
            pltpu.VMEM((CELLS, 28, 2, HEAD, HEAD), BF16),
            pltpu.VMEM((28, 2, HEAD, HEAD), BF16),
            pltpu.VMEM((CELLS, NH, 2, R2, HEAD), F32),
            pltpu.VMEM((CELLS, NH, 8, HEAD), F32),
            pltpu.VMEM((CELLS, NH, HEAD, 8), F32),
            pltpu.VMEM((CELLS, NH, 2, R2, HEAD), F32),
            pltpu.VMEM((CELLS, NH, 2, HEAD, R2), BF16),
            pltpu.VMEM((CELLS, NH, 2, R2, HEAD), F32),
            pltpu.VMEM((2, R2, HEAD), F32),
            pltpu.VMEM((2, R2, HEAD), F32),
            pltpu.VMEM((1, NH, 3, R2, 256), F32),
            *(pltpu.VMEM((NH, 2, 8, WROWS[cell], 512), WIDE[cell]) for cell in range(CELLS)),
            *(pltpu.VMEM((NH, 16, WROWS[cell], 512), WIDE[cell]) for cell in range(CELLS)),
            *(
                pltpu.VMEM(group_shape(cell, group), group_type(cell, group))
                for cell in range(CELLS) for _ in range(2) for group in GROUPS[cell]
            ),
            dma((CELLS, NH, 16)), dma((CELLS, NH, 2, 8)),
            dma((CELLS, NH, 4, 4)), dma((CELLS, NH, 4, 4)),
            dma((CELLS, NH, 4)), dma((CELLS, NH, 4)),
            dma((CELLS, NH, 16)), dma((CELLS, NH, 16)),
            dma((CELLS, 7)), dma((CELLS, 7)), dma((CELLS, 7)),
            dma((CELLS,)), dma((CELLS, 2)), dma((3,)),
        ],
        compiler_params=pltpu.CompilerParams(
            collective_id=0, has_side_effects=True, vmem_limit_bytes=48 * 1024 * 1024
        ),
    )(*(pltpu.with_memory_space_constraint(a, pltpu.HBM) for a in (tokens, wq, wk, wv, wo, wi2, wf2, bias, gain, wp, mem, nrm2, mxs2)))
    res, mem_new, nrm_new, mxs_new = pl.pallas_call(
        flush,
        out_shape=shapes,
        in_specs=[vmem] * 4,
        out_specs=(hbm,) * 4,
        scratch_shapes=[dma((11,))],
        compiler_params=pltpu.CompilerParams(vmem_limit_bytes=1024 * 1024),
    )(*held)
    return res, mem_new, nrm_new.reshape(nrm.shape), mxs_new.transpose(0, 2, 1)


def solution(mesh):
    in_specs = (
        P("tp", "dp"),
        P(None, "dp", "tp"),
        P(None, "dp", "tp"),
        P(None, "dp", "tp"),
        P(None, "dp", "tp"),
        P(None, "dp", None),
        P(None, "dp", None),
        P(None, "tp"),
        P(None, "tp", None),
        P(None, "tp", "dp"),
        P(None, "dp", "tp", None, None),
        P(None, "dp", "tp", None),
        P(None, "dp", "tp"),
    )
    out_specs = (
        P("tp", "dp"),
        P(None, "dp", "tp", None, None),
        P(None, "dp", "tp", None),
        P(None, "dp", "tp"),
    )
    return jax.shard_map(on_device, mesh=mesh, in_specs=in_specs, out_specs=out_specs, check_vma=False)
```
